128 devices in a mesh: grp: 4 (over y, x), ep: 32 (over z, core).
Axes of the slice: x: 2, y: 2, z: 16, core: 2. Of those that a mesh axis runs over, the one named last changes fastest.
The devices are a block of a 8x8x16 slice.
Arguments:
- residual_input: bfloat16 [3072, 2048], P(('grp', 'ep')), parts along dimension 0, may hold values from -6 to 6
- attention_norm_gain: bfloat16 [2048], replicated, may hold values from 0.099609375 to 1.8984375
- receptance_weight: bfloat16 [2048, 1024], P(None, 'ep'), may hold values from -0.125 to 0.125
- key_weight: bfloat16 [2048, 1024], P(None, 'ep'), may hold values from -0.125 to 0.125
- value_weight: bfloat16 [2048, 1024], P(None, 'ep'), may hold values from -0.125 to 0.125
- decay_weight: bfloat16 [2048, 1024], P(None, 'ep'), may hold values from -0.125 to 0.125
- correction_rate_weight: bfloat16 [2048, 1024], P(None, 'ep'), may hold values from -0.125 to 0.125
- output_gate_weight: bfloat16 [2048, 1024], P(None, 'ep'), may hold values from -0.125 to 0.125
- decay_offset: float32 [1024], replicated, may hold values from -3 to 1
- correction_rate_offset: float32 [1024], replicated, may hold values from -1.5 to 1.5
- self_term_weight: float32 [1024], replicated, may hold values from -2 to 2
- head_read_gain: float32 [1024], replicated, may hold values from 0.1 to 1.9
- previous_state: float32 [3072, 16, 4096], P(('grp', 'ep')), parts along dimension 0, may hold values from -4 to 4
- attention_output_weight: bfloat16 [1024, 2048], replicated, may hold values from -0.1875 to 0.1875
- feedforward_norm_gain: bfloat16 [2048], replicated, may hold values from 0.099609375 to 1.8984375
- routes: int32 [3072, 4], P('grp'), parts along dimension 0, may hold values from 0 to 31, all different within a row; in each aligned block of 24 rows (0 to 23, 24 to 47, ...) at most 4 rows name the same one
- routing_weight: float32 [3072, 4], P('grp'), parts along dimension 0, may hold values from 0.2 to 1
- routed_gate_weight: bfloat16 [32, 2048, 512], P('ep'), may hold values from -0.125 to 0.125
- routed_up_weight: bfloat16 [32, 2048, 512], P('ep'), may hold values from -0.125 to 0.125
- routed_down_weight: bfloat16 [32, 512, 2048], P('ep'), may hold values from -0.25 to 0.25
- common_gate_weight: bfloat16 [2048, 512], replicated, may hold values from -0.125 to 0.125
- common_up_weight: bfloat16 [2048, 512], replicated, may hold values from -0.125 to 0.125
- common_down_weight: bfloat16 [512, 2048], replicated, may hold values from -0.25 to 0.25
Outputs:
- hidden_out: bfloat16 [3072, 2048], P(('grp', 'ep')), parts along dimension 0
- next_state: float32 [3072, 16, 4096], P(('grp', 'ep')), parts along dimension 0
The draws below stay inside these ranges and needn't reach their ends.
There are 4 independent parts, one for each index of `grp`. The reference program is written for one: setup_inputs(seed, part) draws one part's arguments, and reference() takes and returns one part's arrays. A program takes and returns all parts, laid end to end along the dimension named above; an argument that names none is the same for every part. Nothing has to cross between parts.
Inputs may be any that keep to these rules, and one draw needn't show every extreme that they name: `routes`: the 4 entries of a row differ. In each aligned block of 24 rows (the tokens of one index of ep) no expert is named by more than 4 rows, a bound that some block reaches.
All inputs are finite; a program needn't handle non-finite values.
Results may differ from the reference program's by a relative error of at most 0.013.
Values may be sent and summed in bfloat16 or wider, within the bound.
A program may use at most 128 MiB of HBM per device.

```python
import math
import jax
import jax.numpy as jnp
import numpy as np
from jax import lax

D = 2048
HEAD_COUNT = 16
HEAD_SIZE = 64
MIXER_WIDTH = 1024
EFF = 512
SFF = 512
EXPERTS = 32
TOPK = 4
CAP = 4
SEQ_DEV = 24
TOKENS = 768
N_EP = 32


def block_levels(key, shape, shards, least, high):
    level, own = 1.0, jax.random.fold_in(key, 6)
    for position, blocks in shards:
        heights = jnp.exp(jax.random.uniform(jax.random.fold_in(own, position), (blocks,), jnp.float32, least / len(shards), high / len(shards)))
        level = level * jnp.repeat(heights, shape[position] // blocks).reshape([-1 if axis == position else 1 for axis in range(len(shape))])
    return level


def routed_block(key, own, number, rows, amount, top, reach, skew):
    sequence = jax.random.permutation(key, amount)
    heavy_load, common = shares(amount, rows * top, reach, skew, True), shares(amount, rows * top, reach, skew, False)
    places = jnp.arange(amount)

    def named(tallies, turn):
        used = int((tallies > 0).sum())
        fixed = max(1, used // 4)
        passed = fixed + (places - fixed + turn * (used - fixed)) % max(1, amount - fixed)
        return jnp.zeros((amount,), jnp.int32).at[sequence[jnp.where(places < fixed, places, passed)]].set(jnp.asarray(tallies, jnp.int32))

    tallies = jnp.where(number % 4 == 0, named(heavy_load, number // 4), named(common, number - number // 4 - 1))
    mixed = jax.random.permutation(jax.random.fold_in(own, 3), amount)
    source_of, receiver = mixed[0:amount // 2 * 2:2], mixed[1:amount // 2 * 2:2]
    room = jnp.minimum(tallies[source_of] - 1, reach - tallies[receiver]) // 2
    room = jnp.where((source_of == sequence[0]) | (receiver == sequence[0]) | (tallies[receiver] == 0), 0, jnp.maximum(room, 0))
    passed = jax.random.randint(jax.random.fold_in(own, 4), (amount // 2,), 0, 1 << 20) % (room + 1)
    tallies = tallies.at[source_of].add(-passed).at[receiver].add(passed)
    members = jnp.searchsorted(jnp.cumsum(tallies), jnp.arange(rows * top), side="right").astype(jnp.int32)
    table = members.reshape(top, rows).T
    table = table[jax.random.permutation(jax.random.fold_in(own, 1), rows)]
    turn = jax.random.randint(jax.random.fold_in(own, 2), (rows, 1), 0, top)
    return jnp.take_along_axis(table, (jnp.arange(top)[None, :] + turn) % top, axis=1)


def shares(count, total, most, slope, full):
    loads = [(1 << 20) // math.isqrt(rank ** slope) + 1 for rank in range(1, count + 1)]
    largest = most if full else min(most, max(-(-total // count), total * loads[0] // sum(loads)))
    least = 1 if total - largest >= count - 1 else 0
    given, rest = [largest] + [least] * (count - 1), total - largest - least * (count - 1)
    while rest > 0:
        candidates = [i for i in range(1, count) if given[i] < largest] or [i for i in range(1, count) if given[i] < most]
        mass, remaining = sum([loads[i] for i in candidates]), rest
        for i in candidates:
            extra = min(most - given[i], max(1, remaining * loads[i] // mass), rest)
            given[i] = given[i] + extra
            rest = rest - extra
    return np.array(given)


def scatter_about(own_key, dims, scale, most, shards=(), kind=jnp.bfloat16):
    level = block_levels(own_key, dims, shards, -0.22, 0.18) if shards else 1.0
    drawn = jax.random.normal(own_key, dims, jnp.float32) * scale * level
    return jnp.minimum(jnp.maximum(drawn, -most), most).astype(kind)


def setup_inputs(seed: int = 0, part: int = 0) -> dict:
    splits = jax.random.split(jax.random.key(seed), 24)
    part_keys = jax.random.split(jax.random.fold_in(splits[23], part), 24)
    residual_input = scatter_about(part_keys[0], (TOKENS, D), 1.0, 6.0, ((0, 32),))
    attention_norm_gain = jnp.clip(1.0 + 0.18 * jax.random.normal(splits[1], (D,), jnp.float32), 0.099609375, 1.8984375).astype(jnp.bfloat16)
    receptance_weight = scatter_about(splits[2], (D, MIXER_WIDTH), D ** -0.5, 0.125, ((1, 32),))
    key_weight = scatter_about(splits[3], (D, MIXER_WIDTH), D ** -0.5, 0.125, ((1, 32),))
    value_weight = scatter_about(splits[4], (D, MIXER_WIDTH), D ** -0.5, 0.125, ((1, 32),))
    decay_weight = scatter_about(splits[5], (D, MIXER_WIDTH), D ** -0.5, 0.125, ((1, 32),))
    correction_rate_weight = scatter_about(splits[6], (D, MIXER_WIDTH), D ** -0.5, 0.125, ((1, 32),))
    output_gate_weight = scatter_about(splits[7], (D, MIXER_WIDTH), D ** -0.5, 0.125, ((1, 32),))
    decay_offset = jnp.clip(jax.random.uniform(splits[8], (MIXER_WIDTH,), jnp.float32, -3.0, 1.0), -3.0, 1.0)
    correction_rate_offset = jnp.clip(jax.random.uniform(splits[9], (MIXER_WIDTH,), jnp.float32, -1.5, 1.5), -1.5, 1.5)
    self_term_weight = scatter_about(splits[10], (MIXER_WIDTH,), 0.15, 2.0, (), jnp.float32)
    head_read_gain = jnp.clip(1.0 + 0.18 * jax.random.normal(splits[11], (MIXER_WIDTH,), jnp.float32), 0.1, 1.9)
    previous_state = scatter_about(part_keys[12], (TOKENS, HEAD_COUNT, HEAD_SIZE * HEAD_SIZE), 0.3, 4.0, ((0, 32),), jnp.float32)
    attention_output_weight = scatter_about(splits[13], (MIXER_WIDTH, D), MIXER_WIDTH ** -0.5, 0.1875)
    feedforward_norm_gain = jnp.clip(1.0 + 0.18 * jax.random.normal(splits[14], (D,), jnp.float32), 0.099609375, 1.8984375).astype(jnp.bfloat16)
    routes_keys = jax.random.split(jax.random.fold_in(part_keys[15], 1), TOKENS // SEQ_DEV)
    routes_turns = jax.random.permutation(jax.random.fold_in(part_keys[15], 3), TOKENS // SEQ_DEV)
    routes = jax.vmap(lambda own, number: routed_block(jax.random.fold_in(part_keys[15], 2), own, number, SEQ_DEV, EXPERTS, TOPK, CAP, 2))(routes_keys, routes_turns).reshape((TOKENS, TOPK))
    routing_weight = jnp.clip(jax.random.uniform(part_keys[16], (TOKENS, TOPK), jnp.float32, 0.2, 1.0), 0.2, 1.0)
    routed_gate_weight = scatter_about(splits[17], (EXPERTS, D, EFF), D ** -0.5, 0.125, ((0, 32),))
    routed_up_weight = scatter_about(splits[18], (EXPERTS, D, EFF), D ** -0.5, 0.125, ((0, 32),))
    routed_down_weight = scatter_about(splits[19], (EXPERTS, EFF, D), EFF ** -0.5, 0.25, ((0, 32),))
    common_gate_weight = scatter_about(splits[20], (D, SFF), D ** -0.5, 0.125)
    common_up_weight = scatter_about(splits[21], (D, SFF), D ** -0.5, 0.125)
    common_down_weight = scatter_about(splits[22], (SFF, D), SFF ** -0.5, 0.25)
    return {"residual_input": residual_input, "attention_norm_gain": attention_norm_gain, "receptance_weight": receptance_weight, "key_weight": key_weight, "value_weight": value_weight, "decay_weight": decay_weight, "correction_rate_weight": correction_rate_weight, "output_gate_weight": output_gate_weight, "decay_offset": decay_offset, "correction_rate_offset": correction_rate_offset, "self_term_weight": self_term_weight, "head_read_gain": head_read_gain, "previous_state": previous_state, "attention_output_weight": attention_output_weight, "feedforward_norm_gain": feedforward_norm_gain, "routes": routes, "routing_weight": routing_weight, "routed_gate_weight": routed_gate_weight, "routed_up_weight": routed_up_weight, "routed_down_weight": routed_down_weight, "common_gate_weight": common_gate_weight, "common_up_weight": common_up_weight, "common_down_weight": common_down_weight}


def rms_norm(value_rows, gain):
    scale = lax.rsqrt(lax.optimization_barrier(jnp.mean(value_rows * value_rows, axis=-1, keepdims=True)) + 1e-06)
    return (value_rows * scale * gain.astype(jnp.float32)).astype(jnp.bfloat16)

def expert_mlp(rows, gate_w, up_w, down_w):
    gate = jnp.dot(rows, gate_w, preferred_element_type=jnp.float32)
    upward = jnp.dot(rows, up_w, preferred_element_type=jnp.float32)
    hidden = (jax.nn.silu(gate) * upward).astype(jnp.bfloat16)
    return jnp.dot(hidden, down_w, preferred_element_type=jnp.float32).astype(jnp.bfloat16)

def attention_mixer(receptance_rows, key_rows, value_rows, decay_logit, rate_logit, gate_logit, decay_offset, correction_rate_offset, self_term_weight, head_read_gain, head_state):
    tally_value = receptance_rows.shape[0]

    def heads(tensor):
        return tensor.astype(jnp.float32).reshape(tally_value, HEAD_COUNT, HEAD_SIZE)
    decay = jnp.exp(-jnp.exp(-jax.nn.softplus(-(decay_offset + decay_logit.astype(jnp.float32))) - 0.5))
    rate = jax.nn.sigmoid(correction_rate_offset + rate_logit.astype(jnp.float32))
    key_head = heads(key_rows)
    rate_head = heads(rate)
    receptance_head = heads(receptance_rows)
    head_value = heads(value_rows)
    unit_key = key_head * lax.rsqrt(1.0 + lax.optimization_barrier(jnp.sum(key_head * key_head, axis=-1, keepdims=True)))
    rate_scaled_key = key_head * rate_head
    removal = unit_key * rate_head
    matrix = head_state.reshape(tally_value, HEAD_COUNT, HEAD_SIZE, HEAD_SIZE)
    recalled = jnp.einsum('nhvk,nhk->nhv', matrix, unit_key, precision=lax.Precision.HIGHEST)
    matrix = matrix * heads(decay)[:, :, None, :] - recalled[..., None] * removal[:, :, None, :] + head_value[..., None] * rate_scaled_key[:, :, None, :]
    read = jnp.einsum('nhvk,nhk->nhv', matrix, receptance_head, precision=lax.Precision.HIGHEST)
    centered = read - lax.optimization_barrier(jnp.mean(read, axis=-1, keepdims=True))
    variance = lax.optimization_barrier(jnp.mean(centered * centered, axis=-1, keepdims=True))
    normed_head_read = centered * lax.rsqrt(variance + 0.00064) * head_read_gain.reshape(HEAD_COUNT, HEAD_SIZE)
    self_term = lax.optimization_barrier(jnp.sum(receptance_head * rate_scaled_key * self_term_weight.reshape(HEAD_COUNT, HEAD_SIZE), axis=-1, keepdims=True)) * head_value
    normed_mixer_input = (normed_head_read + self_term).reshape(tally_value, HEAD_COUNT * HEAD_SIZE) * jax.nn.sigmoid(gate_logit.astype(jnp.float32))
    return (normed_mixer_input.astype(jnp.bfloat16), matrix.reshape(tally_value, HEAD_COUNT, HEAD_SIZE * HEAD_SIZE))

def routed_sum(normed_ffn, routes, routing_weight, routed_gate_weight, routed_up_weight, routed_down_weight):
    tokens = normed_ffn.shape[0]
    limit = N_EP * CAP
    slots = jnp.arange(limit, dtype=jnp.int32)

    def add_expert(expert_id, total):
        match = routes == expert_id
        hit = jnp.any(match, axis=1).astype(jnp.int32)
        weight = lax.optimization_barrier(jnp.sum(jnp.where(match, routing_weight, 0.0), axis=1))
        rank = jnp.cumsum(hit) - hit
        select = (rank[None, :] == slots[:, None]) & (hit[None, :] == 1)
        rows = jnp.dot(select.astype(jnp.bfloat16), normed_ffn, preferred_element_type=jnp.float32).astype(jnp.bfloat16)
        output = expert_mlp(rows, routed_gate_weight[expert_id], routed_up_weight[expert_id], routed_down_weight[expert_id])
        spread = select.astype(jnp.float32).T * weight[:, None]
        return total + jnp.dot(spread, output.astype(jnp.float32), precision=lax.Precision.HIGHEST)
    return lax.fori_loop(0, EXPERTS, add_expert, jnp.zeros((tokens, normed_ffn.shape[1]), jnp.float32))

def reference(residual_input, attention_norm_gain, receptance_weight, key_weight, value_weight, decay_weight, correction_rate_weight, output_gate_weight, decay_offset, correction_rate_offset, self_term_weight, head_read_gain, previous_state, attention_output_weight, feedforward_norm_gain, routes, routing_weight, routed_gate_weight, routed_up_weight, routed_down_weight, common_gate_weight, common_up_weight, common_down_weight):
    normed = rms_norm(residual_input.astype(jnp.float32), attention_norm_gain)

    def apply_projection(weight):
        return jnp.dot(normed, weight, preferred_element_type=jnp.float32).astype(jnp.bfloat16)
    normed_mixer_input, next_state = attention_mixer(apply_projection(receptance_weight), apply_projection(key_weight), apply_projection(value_weight), apply_projection(decay_weight), apply_projection(correction_rate_weight), apply_projection(output_gate_weight), decay_offset, correction_rate_offset, self_term_weight, head_read_gain, previous_state)
    attended = jnp.dot(normed_mixer_input, attention_output_weight, preferred_element_type=jnp.float32).astype(jnp.bfloat16)
    middle = residual_input.astype(jnp.float32) + attended.astype(jnp.float32)
    normed_ffn = rms_norm(middle, feedforward_norm_gain)
    shared = expert_mlp(normed_ffn, common_gate_weight, common_up_weight, common_down_weight)
    routed = routed_sum(normed_ffn, routes, routing_weight, routed_gate_weight, routed_up_weight, routed_down_weight)
    hidden_out = (middle + shared.astype(jnp.float32) + routed).astype(jnp.bfloat16)
    return (hidden_out, next_state)
```

```python
import functools

import jax
import jax.numpy as jnp
from jax import lax
from jax.experimental import pallas as pl
from jax.experimental.pallas import tpu as pltpu
from jax.sharding import PartitionSpec as P

HEAD_COUNT = 16
HEAD_SIZE = 64
ROLES = 6
PIECES = 2
PAD = 32
TOKEN_BLOCK = 8
MESH = pl.DeviceIdType.MESH
F32 = jnp.float32
BF16 = jnp.bfloat16


def iota(shape, dim):
    return lax.broadcasted_iota(jnp.int32, shape, dim)


def norm_rows(rows, gain):
    scale = lax.rsqrt(jnp.mean(rows * rows, axis=-1, keepdims=True) + 1e-06)
    return (rows * scale * gain).astype(BF16)


def mm(a, b):
    return jnp.dot(a, b, preferred_element_type=F32)


def ring_of(size):
    ep = lax.axis_index("ep")
    chips = size // 2
    z, core = ep // 2, lax.rem(ep, 2)

    def at(offset):
        return {"ep": lax.rem(z + offset + chips, chips) * 2 + core}

    return z, core, at, {"ep": z * 2 + 1 - core}


def rcopy(src, dst, send, recv, dev):
    return pltpu.make_async_remote_copy(
        src_ref=src, dst_ref=dst, send_sem=send, recv_sem=recv, device_id=dev, device_id_type=MESH
    )


class Gather:
    def __init__(self, slots, rows, send, recv, at, half):
        self.slots, self.rows, self.send, self.recv, self.at, self.half = slots, rows, send, recv, at, half

    def view(self, s, d, p):
        return self.slots.at[s - 1, d, p, pl.ds(0, self.rows)]

    def copy(self, s, d, p):
        last = isinstance(s, int) and s == self.half
        own = isinstance(s, int) and s == 1
        src = self.view(self.half, 1, p) if own else self.view(s - 1, d, p)
        dst = self.view(s, 0 if last else d, p)
        return rcopy(src, dst, self.send.at[s - 1, d, p], self.recv.at[s - 1, d, p], self.at(1 if d == 0 else -1))

    def has(self, s, d, p):
        return not (isinstance(s, int) and s == self.half) or (p < PIECES // 2) == (d == 0)

    def start(self, s, p):
        for d in range(2):
            if self.has(s, d, p):
                self.copy(s, d, p).start()

    def wait(self, s, p):
        for d in range(2):
            if self.has(s, d, p):
                self.copy(s, d, p).wait_recv()

    def drain(self):
        for s in range(1, self.half + 1):
            for d in range(2):
                for p in range(PIECES):
                    if self.has(s, d, p):
                        self.copy(s, d, p).wait_send()


def project_kernel(
    size,
    x_ref,
    gain_ref,
    w0,
    w1,
    w2,
    w3,
    w4,
    w5,
    eg_ref,
    eu_ref,
    ed_ref,
    out_ref,
    sg_ref,
    su_ref,
    sd_ref,
    raw,
    wx,
    perm,
    slots,
    stage,
    land,
    load_sem,
    swap_send,
    swap_recv,
    g_send,
    g_recv,
    a_send,
    a_recv,
):
    z, core, at, sibling = ring_of(size)
    rows, width = x_ref.shape
    half = size // 4
    part = width // PIECES
    cols = w0.shape[1]
    loads = [pltpu.make_async_copy(w, raw.at[i], load_sem.at[i]) for i, w in enumerate((w0, w1, w2, w3, w4, w5))]
    for load in loads:
        load.start()
    barrier = pltpu.get_barrier_semaphore()
    for dev in (at(-1), at(1), sibling):
        pl.semaphore_signal(barrier, inc=1, device_id=dev, device_id_type=MESH)
    normed = norm_rows(x_ref[...].astype(F32), gain_ref[...].astype(F32))
    for p in range(PIECES):
        slots[half - 1, 1, p, 0:rows] = normed[:, p * part : (p + 1) * part]
    pl.semaphore_wait(barrier, 3)
    gather = Gather(slots, rows, g_send, g_recv, at, half)
    for p in range(PIECES):
        gather.start(1, p)
    swaps = [
        rcopy(src, dst, swap_send.at[i + 1], swap_recv.at[i + 1], sibling)
        for i, (src, dst) in enumerate(((eg_ref, sg_ref), (eu_ref, su_ref), (ed_ref, sd_ref)))
    ]
    for i, load in enumerate(loads):
        load.wait()
        wx[core, :, i * cols : (i + 1) * cols] = raw[i]
    swap = rcopy(wx.at[core], wx.at[core], swap_send.at[0], swap_recv.at[0], sibling)
    swap.start()
    for copy in swaps:
        copy.start()
    count = ROLES * cols
    for k in range(2):
        i, j = iota((count, 2 * count), 0), iota((count, 2 * count), 1)
        role = (i * (65536 // cols + 1)) >> 16
        perm[k] = jnp.where(j == i + role * cols + k * cols, 1.0, 0.0).astype(BF16)
    other = rcopy(wx.at[1 - core], wx.at[1 - core], swap_send.at[0], swap_recv.at[0], sibling)

    def project(s):
        done = None
        for k in range(2):
            acc = None
            for p in range(PIECES):
                term = mm(slots[s - 1, :, p].reshape(2 * PAD, part), wx[k, p * part : (p + 1) * part, :])
                acc = term if acc is None else acc + term
            moved = mm(acc.astype(BF16), perm[k])
            done = moved if done is None else done + moved
        stage[s - 1] = done.astype(BF16).reshape(2, PAD, 2 * count)

    def deliver(s, d):
        return rcopy(
            stage.at[s - 1, d, pl.ds(0, rows)], land.at[z], a_send.at[s - 1, d], a_recv.at[s - 1, d], at(-s if d == 0 else s)
        )

    for p in range(PIECES):
        gather.wait(1, p)
        gather.start(2, p)
    other.wait_recv()
    project(1)
    deliver(1, 0).start()
    deliver(1, 1).start()

    def step(s, carry):
        for p in range(PIECES):
            gather.wait(s, p)
            gather.start(s + 1, p)
        project(s)
        deliver(s, 0).start()
        deliver(s, 1).start()
        return carry

    lax.fori_loop(2, half - 1, step, 0)
    for p in range(PIECES):
        gather.wait(half - 1, p)
        gather.start(half, p)
    project(half - 1)
    deliver(half - 1, 0).start()
    deliver(half - 1, 1).start()
    for p in range(PIECES):
        gather.wait(half, p)
    project(half)
    deliver(half, 0).start()
    land[z] = stage[half - 1, 1, 0:rows]
    gather.drain()
    swap.wait_send()
    for copy in swaps:
        copy.wait()
    for s in range(1, half + 1):
        for d in range(2):
            if s < half or d == 0:
                deliver(s, d).wait()
    out_ref[...] = land[...]


def sigmoid(v):
    return 1.0 / (1.0 + jnp.exp(-v))


def state_kernel(
    r_ref, prm_ref, x_ref, wo_ref, s_ref, ns_ref, mid_ref, rt, tt, vecs, vals, gate, self_s, blk, exp_m, red_m, mixed, xcat, wo, wo_sem
):
    step, steps = pl.program_id(0), pl.num_programs(0)
    tokens = x_ref.shape[0]
    total = tokens * HEAD_COUNT
    two = 2 * HEAD_SIZE
    load = pltpu.make_async_copy(wo_ref, wo, wo_sem)

    @pl.when(step == 0)
    def _():
        load.start()
        for i in range(3):
            rt[i] = r_ref[:, :, i * two : (i + 1) * two].astype(F32).reshape(total, two)
        for i in range(3):
            for t in range(tokens):
                tt[i, t * HEAD_COUNT : (t + 1) * HEAD_COUNT] = rt[i, pl.ds(t, HEAD_COUNT, stride=tokens), :]
        low = iota((total, two), 1) < HEAD_SIZE

        def split(i):
            a = tt[i]
            b = pltpu.roll(a, HEAD_SIZE, 1)
            return jnp.where(low, a, b), jnp.where(low, b, a)

        def param(i):
            v = prm_ref[i]
            v = jnp.concatenate([v, v], axis=1)
            return jnp.broadcast_to(v[None], (tokens, HEAD_COUNT, two)).reshape(total, two)

        rr, kk = split(0)
        vv, dd = split(1)
        ta, gg = split(2)
        decay = jnp.exp(-0.6065306597126334 * sigmoid(param(0) + dd))
        rate = sigmoid(param(1) + ta)
        rs = lax.rsqrt(1.0 + 0.5 * jnp.sum(kk * kk, axis=-1, keepdims=True))
        sk = kk * rate
        vecs[0] = -(rs * rs) * kk
        vecs[1] = decay
        vecs[2] = sk
        vecs[3] = rr
        vals[...] = vv.astype(BF16)
        self_s[...] = 0.5 * jnp.sum(rr * sk * param(2), axis=-1, keepdims=True) * vv
        gate[...] = sigmoid(gg)
        i, j = iota((256, 256), 0), iota((256, 256), 1)
        blk[...] = jnp.where((i >> 6) == (j >> 6), 1.0, 0.0).astype(BF16)
        i, j = iota((two, HEAD_SIZE * HEAD_SIZE), 0), iota((two, HEAD_SIZE * HEAD_SIZE), 1)
        exp_m[...] = jnp.where((j >> 6) == i, 1.0, 0.0).astype(BF16)
        i, j = iota((HEAD_SIZE * HEAD_SIZE, two), 0), iota((HEAD_SIZE * HEAD_SIZE, two), 1)
        red_m[...] = jnp.where((i >> 6) == (j & (HEAD_SIZE - 1)), 1.0, 0.0).astype(BF16)

    block = s_ref.shape[0]
    m = block * HEAD_COUNT
    at = pl.ds(pl.multiple_of(step * m, m), m)

    def wide(i):
        v = vecs[i, at, :]
        return jnp.concatenate([v, v], axis=1)

    u2, dec, sk, rr = wide(0), wide(1), wide(2), wide(3)
    val = vals[at, :]
    read = jnp.zeros((m, two), F32)
    for jj in range(HEAD_SIZE * HEAD_SIZE // 256):
        ls = slice(jj * 256, (jj + 1) * 256)
        s = s_ref[:, :, ls].reshape(m, 256)
        comb = mm((s * u2).astype(BF16), blk[...]) + mm(val, exp_m[:, ls])
        new = s * dec + sk * comb
        ns_ref[:, :, ls] = new.reshape(block, HEAD_COUNT, 256)
        read = read + mm((new * rr).astype(BF16), red_m[ls, :])
    centered = read - jnp.mean(read, axis=-1, keepdims=True)
    var = jnp.mean(centered * centered, axis=-1, keepdims=True)
    gain = jnp.concatenate([prm_ref[3], prm_ref[3]], axis=1)
    gain = jnp.broadcast_to(gain[None], (block, HEAD_COUNT, two)).reshape(m, two)
    mixed[at, :] = (centered * lax.rsqrt(var + 0.00064) * gain + self_s[at, :]) * gate[at, :]

    @pl.when(step == steps - 1)
    def _():
        low = iota((tokens, two), 1) < HEAD_SIZE
        for h in range(0, HEAD_COUNT, 2):
            a = mixed[pl.ds(h, tokens, stride=HEAD_COUNT), :]
            b = mixed[pl.ds(h + 1, tokens, stride=HEAD_COUNT), :]
            xcat[:, h * HEAD_SIZE : h * HEAD_SIZE + two] = jnp.where(low, a, b)
        load.wait()
        attended = mm(xcat[...].astype(BF16), wo[...]).astype(BF16)
        mid_ref[...] = x_ref[...].astype(F32) + attended.astype(F32)


def silu(v):
    return v * sigmoid(v)


def expert_kernel(
    size,
    mid_ref,
    gain_ref,
    routes_ref,
    rweight_ref,
    eg_ref,
    eu_ref,
    ed_ref,
    sg_ref,
    su_ref,
    sd_ref,
    cg_ref,
    cu_ref,
    cd_ref,
    out_ref,
    wg,
    wu,
    wd,
    slots,
    contrib,
    arrive,
    hidden,
    first,
    coef,
    base,
    load_sem,
    g_send,
    g_recv,
    r_send,
    r_recv,
):
    z, core, at, sibling = ring_of(size)
    rows, width = mid_ref.shape
    half = size // 4
    part = width // PIECES
    loads = []
    for i, group in enumerate(((cg_ref, cu_ref, cd_ref), (eg_ref.at[0], eu_ref.at[0], ed_ref.at[0]), (sg_ref.at[0], su_ref.at[0], sd_ref.at[0]))):
        for j, (src, dst) in enumerate(zip(group, (wg, wu, wd))):
            loads.append(pltpu.make_async_copy(src, dst.at[i], load_sem.at[i, j]))
    for load in loads:
        load.start()
    barrier = pltpu.get_barrier_semaphore()
    for dev in (at(-1), at(1)):
        pl.semaphore_signal(barrier, inc=1, device_id=dev, device_id_type=MESH)
    normed = norm_rows(mid_ref[...], gain_ref[...].astype(F32))
    for p in range(PIECES):
        slots[half - 1, 1, p, 0:rows] = normed[:, p * part : (p + 1) * part]
    pl.semaphore_wait(barrier, 2)
    gather = Gather(slots, rows, g_send, g_recv, at, half)
    for p in range(PIECES):
        gather.start(1, p)

    ep = lax.axis_index("ep")
    for e, expert in enumerate((ep, sibling["ep"])):
        for s in range(1, half + 1):
            for d in range(2):
                chip = at(0 if (s == half and d == 1) else (-s if d == 0 else s))["ep"]
                where = pl.ds(pl.multiple_of(chip * rows, 8), rows)
                hit = routes_ref[where, :] == expert
                w = jnp.sum(jnp.where(hit, rweight_ref[where, :], 0.0), axis=-1, keepdims=True)
                coef[e, ((s - 1) * 2 + d) * PAD : ((s - 1) * 2 + d) * PAD + rows] = w

    def up(e, rows_of, count):
        gate = up_ = None
        for p in range(PIECES):
            r = rows_of(p)
            ks = slice(p * part, (p + 1) * part)
            g, u = mm(r, wg[e, ks, :]), mm(r, wu[e, ks, :])
            gate, up_ = (g, u) if gate is None else (gate + g, up_ + u)
        hidden[0:count] = (silu(gate) * up_).astype(BF16)

    def shared_up():
        for load in loads[0:2]:
            load.wait()
        up(0, lambda p: slots[half - 1, 1, p], PAD)

    def shared_down():
        loads[2].wait()
        out = mm(hidden[0:PAD], wd[0])[0:rows]
        base[...] = mid_ref[...] + out.astype(BF16).astype(F32)

    def expert_up(e, b):
        up(e + 1, lambda p: slots[pl.ds(2 * b, 2), :, p].reshape(4 * PAD, part), 4 * PAD)

    def expert_down(e, b):
        cf = coef[e, pl.ds(pl.multiple_of(b * (4 * PAD), 4 * PAD), 4 * PAD), :]
        for p in range(PIECES):
            for c in range(0, part, 512):
                o = mm(hidden[...], wd[e + 1, :, p * part + c : p * part + c + 512])
                o = o.astype(BF16).astype(F32) * cf
                if e == 0:
                    first[:, p * part + c : p * part + c + 512] = o
                else:
                    o = o + first[:, p * part + c : p * part + c + 512]
                    contrib[pl.ds(2 * b, 2), :, p, :, c : c + 512] = o.astype(BF16).reshape(2, 2, PAD, 512)

    def forward(s, p):
        gather.wait(s, p)
        if not (isinstance(s, int) and s == half):
            gather.start(s + 1, p)

    def turn(s, work):
        for i in range(2):
            for p in range(i * PIECES // 2, (i + 1) * PIECES // 2):
                forward(s, p)
            work[i]()

    turn(1, (shared_up, shared_down))
    for p in range(PIECES):
        forward(2, p)
    for load in loads[3:]:
        load.wait()

    def pair(b, carry):
        for e in range(2):
            turn(2 * b + 3 + e, (functools.partial(expert_up, e, b), functools.partial(expert_down, e, b)))
        return carry

    lax.fori_loop(0, half // 2 - 2, pair, 0)
    b = half // 2 - 2
    for e in range(2):
        turn(2 * b + 3 + e, (functools.partial(expert_up, e, b), functools.partial(expert_down, e, b)))
    b = half // 2 - 1
    for e in range(2):
        expert_up(e, b)
        expert_down(e, b)

    def passed(t, d, p, source):
        return rcopy(
            contrib.at[source - 1, 0 if isinstance(source, int) and source == half else d, p, pl.ds(0, rows)],
            arrive.at[t, d, p, pl.ds(0, rows)],
            r_send.at[t, d, p],
            r_recv.at[t, d, p],
            at(-1 if d == 0 else 1),
        )

    def begins(d, p):
        return (p < PIECES // 2) == (d == 0)

    for p in range(PIECES):
        for d in range(2):
            if begins(d, p):
                passed(0, d, p, half).start()
            else:
                passed(1, d, p, half - 1).start()

    def relay(t, d, p):
        passed(t - 1, d, p, half - t).wait_recv()
        mine = contrib[half - t - 1, d, p, 0:rows].astype(F32)
        contrib[half - t - 1, d, p, 0:rows] = (mine + arrive[t - 1, d, p, 0:rows].astype(F32)).astype(BF16)
        passed(t, d, p, half - t).start()

    for p in range(PIECES):
        for d in range(2):
            if begins(d, p):
                relay(1, d, p)

    def hop(t, carry):
        for p in range(PIECES):
            for d in range(2):
                relay(t, d, p)
        return carry

    lax.fori_loop(2, half, hop, 0)
    for p in range(PIECES):
        for d in range(2):
            passed(half - 1, d, p, 1).wait_recv()
        got = arrive[half - 1, 0, p, 0:rows].astype(F32) + arrive[half - 1, 1, p, 0:rows].astype(F32)
        total = base[:, p * part : (p + 1) * part] + contrib[half - 1, 1, p, 0:rows].astype(F32) + got
        out_ref[:, p * part : (p + 1) * part] = total.astype(BF16)
    gather.drain()
    for p in range(PIECES):
        for d in range(2):
            for t in range(half):
                if t > 0 or begins(d, p):
                    passed(t, d, p, half - t).wait_send()


VM = pl.BlockSpec(memory_space=pltpu.VMEM)
ANY = pl.BlockSpec(memory_space=pl.ANY)
DMA = pltpu.SemaphoreType.DMA


def per_device(
    residual_input,
    attention_norm_gain,
    receptance_weight,
    key_weight,
    value_weight,
    decay_weight,
    correction_rate_weight,
    output_gate_weight,
    decay_offset,
    correction_rate_offset,
    self_term_weight,
    head_read_gain,
    previous_state,
    attention_output_weight,
    feedforward_norm_gain,
    routes,
    routing_weight,
    routed_gate_weight,
    routed_up_weight,
    routed_down_weight,
    common_gate_weight,
    common_up_weight,
    common_down_weight,
):
    size = lax.axis_size("ep")
    half = size // 4
    rows, width = residual_input.shape
    part = width // PIECES
    cols = receptance_weight.shape[1]
    lanes = ROLES * cols
    big = pltpu.CompilerParams
    landed, sib_gate, sib_up, sib_down = pl.pallas_call(
        functools.partial(project_kernel, size),
        out_shape=(
            jax.ShapeDtypeStruct((size // 2, rows, 2 * lanes), BF16),
            jax.ShapeDtypeStruct(routed_gate_weight.shape, BF16),
            jax.ShapeDtypeStruct(routed_up_weight.shape, BF16),
            jax.ShapeDtypeStruct(routed_down_weight.shape, BF16),
        ),
        in_specs=[VM, VM] + [ANY] * 9,
        out_specs=(VM, ANY, ANY, ANY),
        scratch_shapes=[
            pltpu.VMEM((ROLES, width, cols), BF16),
            pltpu.VMEM((2, width, lanes), BF16),
            pltpu.VMEM((2, lanes, 2 * lanes), BF16),
            pltpu.VMEM((half, 2, PIECES, PAD, part), BF16),
            pltpu.VMEM((half, 2, PAD, 2 * lanes), BF16),
            pltpu.VMEM((size // 2, rows, 2 * lanes), BF16),
            DMA((ROLES,)),
            DMA((4,)),
            DMA((4,)),
            DMA((half, 2, PIECES)),
            DMA((half, 2, PIECES)),
            DMA((half, 2)),
            DMA((half, 2)),
        ],
        compiler_params=big(collective_id=0, has_side_effects=True, vmem_limit_bytes=40 << 20),
        name="project",
    )(
        residual_input,
        attention_norm_gain.reshape(1, width),
        receptance_weight,
        key_weight,
        value_weight,
        decay_weight,
        correction_rate_weight,
        output_gate_weight,
        routed_gate_weight,
        routed_up_weight,
        routed_down_weight,
    )
    prm = jnp.stack((decay_offset, correction_rate_offset, self_term_weight, head_read_gain)).reshape(
        4, HEAD_COUNT, HEAD_SIZE
    )
    total = rows * HEAD_COUNT
    two = 2 * HEAD_SIZE
    square = HEAD_SIZE * HEAD_SIZE
    block = pl.BlockSpec((TOKEN_BLOCK, HEAD_COUNT, square), lambda i: (i, 0, 0))

    def whole(shape):
        return pl.BlockSpec(shape, lambda i: (0,) * len(shape))

    next_state, middle = pl.pallas_call(
        state_kernel,
        grid=(rows // TOKEN_BLOCK,),
        out_shape=(
            jax.ShapeDtypeStruct(previous_state.shape, F32),
            jax.ShapeDtypeStruct((rows, width), F32),
        ),
        in_specs=[whole(landed.shape), whole(prm.shape), whole(residual_input.shape), ANY, block],
        out_specs=(block, whole((rows, width))),
        scratch_shapes=[
            pltpu.VMEM((3, total, two), F32),
            pltpu.VMEM((3, total, two), F32),
            pltpu.VMEM((4, total, two), F32),
            pltpu.VMEM((total, two), BF16),
            pltpu.VMEM((total, two), F32),
            pltpu.VMEM((total, two), F32),
            pltpu.VMEM((256, 256), BF16),
            pltpu.VMEM((two, square), BF16),
            pltpu.VMEM((square, two), BF16),
            pltpu.VMEM((total, two), F32),
            pltpu.VMEM((rows, HEAD_COUNT * HEAD_SIZE), F32),
            pltpu.VMEM(attention_output_weight.shape, BF16),
            DMA,
        ],
        compiler_params=big(dimension_semantics=("arbitrary",), vmem_limit_bytes=40 << 20),
        name="state",
    )(landed, prm, residual_input, attention_output_weight, previous_state)
    inner = routed_gate_weight.shape[2]
    hidden_out = pl.pallas_call(
        functools.partial(expert_kernel, size),
        out_shape=jax.ShapeDtypeStruct((rows, width), BF16),
        in_specs=[VM] * 4 + [ANY] * 9,
        out_specs=VM,
        scratch_shapes=[
            pltpu.VMEM((3, width, inner), BF16),
            pltpu.VMEM((3, width, inner), BF16),
            pltpu.VMEM((3, inner, width), BF16),
            pltpu.VMEM((half, 2, PIECES, PAD, part), BF16),
            pltpu.VMEM((half, 2, PIECES, PAD, part), BF16),
            pltpu.VMEM((half, 2, PIECES, PAD, part), BF16),
            pltpu.VMEM((4 * PAD, inner), BF16),
            pltpu.VMEM((4 * PAD, width), F32),
            pltpu.VMEM((2, 2 * half * PAD, 1), F32),
            pltpu.VMEM((rows, width), F32),
            DMA((3, 3)),
            DMA((half, 2, PIECES)),
            DMA((half, 2, PIECES)),
            DMA((half, 2, PIECES)),
            DMA((half, 2, PIECES)),
        ],
        compiler_params=big(collective_id=1, has_side_effects=True, vmem_limit_bytes=52 << 20),
        name="experts",
    )(
        middle,
        feedforward_norm_gain.reshape(1, width),
        routes,
        routing_weight,
        routed_gate_weight,
        routed_up_weight,
        routed_down_weight,
        sib_gate,
        sib_up,
        sib_down,
        common_gate_weight,
        common_up_weight,
        common_down_weight,
    )
    return (hidden_out, next_state)


def solution(mesh):
    return jax.shard_map(
        per_device,
        mesh=mesh,
        in_specs=(
            P(("grp", "ep"), None),
            P(),
            P(None, "ep"),
            P(None, "ep"),
            P(None, "ep"),
            P(None, "ep"),
            P(None, "ep"),
            P(None, "ep"),
            P(),
            P(),
            P(),
            P(),
            P(("grp", "ep"), None, None),
            P(),
            P(),
            P("grp", None),
            P("grp", None),
            P("ep", None, None),
            P("ep", None, None),
            P("ep", None, None),
            P(),
            P(),
            P(),
        ),
        out_specs=(P(("grp", "ep"), None), P(("grp", "ep"), None, None)),
        check_vma=False,
    )
```

```python
import functools

import jax
import jax.numpy as jnp
from jax import lax
from jax.experimental import pallas as pl
from jax.experimental.pallas import tpu as pltpu
from jax.sharding import PartitionSpec as P

HEAD_COUNT = 16
HEAD_SIZE = 64
ROLES = 6
PIECES = 4
PAD = 32
TOKEN_BLOCK = 8
MESH = pl.DeviceIdType.MESH
F32 = jnp.float32
BF16 = jnp.bfloat16


def iota(shape, dim):
    return lax.broadcasted_iota(jnp.int32, shape, dim)


def norm_rows(rows, gain):
    scale = lax.rsqrt(jnp.mean(rows * rows, axis=-1, keepdims=True) + 1e-06)
    return (rows * scale * gain).astype(BF16)


def mm(a, b):
    return jnp.dot(a, b, preferred_element_type=F32)


def ring_of(size):
    ep = lax.axis_index("ep")
    chips = size // 2
    z, core = ep // 2, lax.rem(ep, 2)

    def at(offset):
        return {"ep": lax.rem(z + offset + chips, chips) * 2 + core}

    return z, core, at, {"ep": z * 2 + 1 - core}


def rcopy(src, dst, send, recv, dev):
    return pltpu.make_async_remote_copy(
        src_ref=src, dst_ref=dst, send_sem=send, recv_sem=recv, device_id=dev, device_id_type=MESH
    )


class Gather:
    def __init__(self, slots, rows, send, recv, at, half):
        self.slots, self.rows, self.send, self.recv, self.at, self.half = slots, rows, send, recv, at, half

    def view(self, s, d, p):
        return self.slots.at[s - 1, d, p, pl.ds(0, self.rows)]

    def copy(self, s, d, p):
        last = isinstance(s, int) and s == self.half
        own = isinstance(s, int) and s == 1
        src = self.view(self.half, 1, p) if own else self.view(s - 1, d, p)
        dst = self.view(s, 0 if last else d, p)
        return rcopy(src, dst, self.send.at[s - 1, d, p], self.recv.at[s - 1, d, p], self.at(1 if d == 0 else -1))

    def has(self, s, d, p):
        return not (isinstance(s, int) and s == self.half) or (p < PIECES // 2) == (d == 0)

    def start(self, s, p):
        for d in range(2):
            if self.has(s, d, p):
                self.copy(s, d, p).start()

    def wait(self, s, p):
        for d in range(2):
            if self.has(s, d, p):
                self.copy(s, d, p).wait_recv()

    def drain(self):
        for s in range(1, self.half + 1):
            for d in range(2):
                for p in range(PIECES):
                    if self.has(s, d, p):
                        self.copy(s, d, p).wait_send()


def project_kernel(
    size,
    x_ref,
    gain_ref,
    w0,
    w1,
    w2,
    w3,
    w4,
    w5,
    eg_ref,
    eu_ref,
    ed_ref,
    out_ref,
    blk_ref,
    exp_ref,
    red_ref,
    sg_ref,
    su_ref,
    sd_ref,
    wide,
    tall,
    slots,
    stage,
    land,
    load_sem,
    swap_send,
    swap_recv,
    g_send,
    g_recv,
    a_send,
    a_recv,
):
    z, core, at, sibling = ring_of(size)
    rows, width = x_ref.shape
    half = size // 4
    part = width // PIECES
    cols = w0.shape[0]
    mine, others = [], []
    for i in range(ROLES):
        mine.append(wide.at[pl.ds(pl.multiple_of(i * 2 * cols + core * cols, cols), cols)])
        others.append(wide.at[pl.ds(pl.multiple_of(i * 2 * cols + (1 - core) * cols, cols), cols)])
    weights = (w0, w1, w2, w3, w4, w5)
    loads = [pltpu.make_async_copy(w, mine[i], load_sem.at[i]) for i, w in enumerate(weights)]
    for load in loads:
        load.start()
    barrier = pltpu.get_barrier_semaphore()
    for dev in (at(-1), at(1), sibling):
        pl.semaphore_signal(barrier, inc=1, device_id=dev, device_id_type=MESH)
    normed = norm_rows(x_ref[...].astype(F32), gain_ref[...].astype(F32))
    for p in range(PIECES):
        slots[half - 1, 1, p, 0:rows] = normed[:, p * part : (p + 1) * part]
    pl.semaphore_wait(barrier, 3)
    gather = Gather(slots, rows, g_send, g_recv, at, half)
    for p in range(PIECES):
        gather.start(1, p)
    swaps = [rcopy(w, mine[i], swap_send.at[i], swap_recv.at[i], sibling) for i, w in enumerate(weights)]
    swaps += [
        rcopy(src, dst, swap_send.at[ROLES + i], swap_recv.at[ROLES + i], sibling)
        for i, (src, dst) in enumerate(((eg_ref, sg_ref), (eu_ref, su_ref), (ed_ref, sd_ref)))
    ]
    for copy in swaps:
        copy.start()
    square, two = red_ref.shape
    side = blk_ref.shape[0]
    i, j = iota((side, side), 0), iota((side, side), 1)
    blk_ref[...] = jnp.where((i >> 6) == (j >> 6), 1.0, 0.0).astype(BF16)
    i, j = iota((two, square), 0), iota((two, square), 1)
    exp_ref[...] = jnp.where((j >> 6) == i, 1.0, 0.0).astype(BF16)
    i, j = iota((square, two), 0), iota((square, two), 1)
    red_ref[...] = jnp.where((i >> 6) == (j & (HEAD_SIZE - 1)), 1.0, 0.0).astype(BF16)
    for i in range(ROLES):
        loads[i].wait()
        rcopy(weights[i], others[i], swap_send.at[i], swap_recv.at[i], sibling).wait_recv()
    for k in range(0, width, 256):
        tall[k : k + 256, :] = wide[:, k : k + 256].T

    def advance(s):
        acc = None
        for p in range(PIECES):
            gather.wait(s, p)
            if not (isinstance(s, int) and s == half):
                gather.start(s + 1, p)
            term = mm(slots[s - 1, :, p].reshape(2 * PAD, part), tall[p * part : (p + 1) * part, :])
            acc = term if acc is None else acc + term
        stage[s - 1] = acc.astype(BF16).reshape(2, PAD, 2 * ROLES * cols)

    def deliver(s, d):
        return rcopy(
            stage.at[s - 1, d, pl.ds(0, rows)], land.at[z], a_send.at[s - 1, d], a_recv.at[s - 1, d], at(-s if d == 0 else s)
        )

    def step(s, carry):
        advance(s)
        deliver(s, 0).start()
        deliver(s, 1).start()
        return carry

    step(1, 0)
    lax.fori_loop(2, half - 1, step, 0)
    step(half - 1, 0)
    advance(half)
    deliver(half, 0).start()
    land[z] = stage[half - 1, 1, 0:rows]
    gather.drain()
    for i, copy in enumerate(swaps):
        copy.wait_send()
        if i >= ROLES:
            copy.wait_recv()
    for s in range(1, half + 1):
        for d in range(2):
            if s < half or d == 0:
                deliver(s, d).wait()
    out_ref[...] = land[...]


def sigmoid(v):
    return 1.0 / (1.0 + jnp.exp(-v))


def state_kernel(
    r_ref,
    blk,
    exp_m,
    red_m,
    prm_ref,
    x_ref,
    wo_ref,
    s_ref,
    ns_ref,
    mid_ref,
    olds,
    news,
    wo,
    rt,
    tt,
    vecs,
    vals,
    gate,
    self_s,
    mixed,
    xcat,
    in_sem,
    out_sem,
    wo_sem,
):
    tokens = x_ref.shape[0]
    total = tokens * HEAD_COUNT
    two = 2 * HEAD_SIZE
    block = TOKEN_BLOCK
    m = block * HEAD_COUNT

    def load(i):
        return pltpu.make_async_copy(s_ref.at[pl.ds(i * block, block)], olds.at[i], in_sem.at[i])

    def store(i):
        return pltpu.make_async_copy(news.at[i], ns_ref.at[pl.ds(i * block, block)], out_sem.at[i])

    wo_load = pltpu.make_async_copy(wo_ref, wo, wo_sem)
    for i in range(tokens // block):
        load(i).start()
    wo_load.start()
    for i in range(3):
        rt[i] = r_ref[:, :, i * two : (i + 1) * two].astype(F32).reshape(total, two)
    for i in range(3):
        for t in range(tokens):
            tt[i, t * HEAD_COUNT : (t + 1) * HEAD_COUNT] = rt[i, pl.ds(t, HEAD_COUNT, stride=tokens), :]
    low = iota((total, two), 1) < HEAD_SIZE

    def split(i):
        a = tt[i]
        b = pltpu.roll(a, HEAD_SIZE, 1)
        return jnp.where(low, a, b), jnp.where(low, b, a)

    def param(i, count):
        v = jnp.concatenate([prm_ref[i], prm_ref[i]], axis=1)
        return jnp.broadcast_to(v[None], (count, HEAD_COUNT, two)).reshape(count * HEAD_COUNT, two)

    rr, kk = split(0)
    vv, dd = split(1)
    ta, gg = split(2)
    rate = sigmoid(param(1, tokens) + ta)
    rs = lax.rsqrt(1.0 + 0.5 * jnp.sum(kk * kk, axis=-1, keepdims=True))
    sk = kk * rate
    vecs[0] = -(rs * rs) * kk
    vecs[1] = jnp.exp(-0.6065306597126334 * sigmoid(param(0, tokens) + dd))
    vecs[2] = sk
    vecs[3] = rr
    vals[...] = vv.astype(BF16)
    self_s[...] = 0.5 * jnp.sum(rr * sk * param(2, tokens), axis=-1, keepdims=True) * vv
    gate[...] = sigmoid(gg)

    def update(i, carry):
        load(i).wait()
        at = pl.ds(pl.multiple_of(i * m, m), m)

        def wide(k):
            v = vecs[k, at, :]
            return jnp.concatenate([v, v], axis=1)

        u2, dec, sk, rr = wide(0), wide(1), wide(2), wide(3)
        val = vals[at, :]
        read = jnp.zeros((m, two), F32)
        for jj in range(HEAD_SIZE * HEAD_SIZE // 256):
            ls = slice(jj * 256, (jj + 1) * 256)
            s = olds[i, :, :, ls].reshape(m, 256)
            comb = mm((s * u2).astype(BF16), blk[...]) + mm(val, exp_m[:, ls])
            new = s * dec + sk * comb
            news[i, :, :, ls] = new.reshape(block, HEAD_COUNT, 256)
            read = read + mm((new * rr).astype(BF16), red_m[ls, :])
        store(i).start()
        centered = read - jnp.mean(read, axis=-1, keepdims=True)
        var = jnp.mean(centered * centered, axis=-1, keepdims=True)
        mixed[at, :] = (centered * lax.rsqrt(var + 0.00064) * param(3, block) + self_s[at, :]) * gate[at, :]
        return carry

    lax.fori_loop(0, tokens // block, update, 0)
    low = iota((tokens, two), 1) < HEAD_SIZE
    for h in range(0, HEAD_COUNT, 2):
        a = mixed[pl.ds(h, tokens, stride=HEAD_COUNT), :]
        b = mixed[pl.ds(h + 1, tokens, stride=HEAD_COUNT), :]
        xcat[:, h * HEAD_SIZE : h * HEAD_SIZE + two] = jnp.where(low, a, b)
    wo_load.wait()
    attended = mm(xcat[...].astype(BF16), wo[...]).astype(BF16)
    mid_ref[...] = x_ref[...].astype(F32) + attended.astype(F32)
    for i in range(tokens // block):
        store(i).wait()


def silu(v):
    return v * sigmoid(v)


def expert_kernel(
    size,
    mid_ref,
    gain_ref,
    routes_ref,
    rweight_ref,
    eg_ref,
    eu_ref,
    ed_ref,
    sg_ref,
    su_ref,
    sd_ref,
    cg_ref,
    cu_ref,
    cd_ref,
    out_ref,
    wg,
    wu,
    wd,
    slots,
    contrib,
    arrive,
    hidden,
    first,
    coef,
    base,
    load_sem,
    g_send,
    g_recv,
    r_send,
    r_recv,
):
    z, core, at, sibling = ring_of(size)
    rows, width = mid_ref.shape
    half = size // 4
    part = width // PIECES
    loads = []
    for i, group in enumerate(((cg_ref, cu_ref, cd_ref), (eg_ref.at[0], eu_ref.at[0], ed_ref.at[0]), (sg_ref.at[0], su_ref.at[0], sd_ref.at[0]))):
        for j, (src, dst) in enumerate(zip(group, (wg, wu, wd))):
            loads.append(pltpu.make_async_copy(src, dst.at[i], load_sem.at[i, j]))
    for load in loads:
        load.start()
    barrier = pltpu.get_barrier_semaphore()
    for dev in (at(-1), at(1)):
        pl.semaphore_signal(barrier, inc=1, device_id=dev, device_id_type=MESH)
    normed = norm_rows(mid_ref[...], gain_ref[...].astype(F32))
    for p in range(PIECES):
        slots[half - 1, 1, p, 0:rows] = normed[:, p * part : (p + 1) * part]
    pl.semaphore_wait(barrier, 2)
    gather = Gather(slots, rows, g_send, g_recv, at, half)
    for p in range(PIECES):
        gather.start(1, p)

    ep = lax.axis_index("ep")
    for e, expert in enumerate((ep, sibling["ep"])):
        for s in range(1, half + 1):
            for d in range(2):
                chip = at(0 if (s == half and d == 1) else (-s if d == 0 else s))["ep"]
                where = pl.ds(pl.multiple_of(chip * rows, 8), rows)
                hit = routes_ref[where, :] == expert
                w = jnp.sum(jnp.where(hit, rweight_ref[where, :], 0.0), axis=-1, keepdims=True)
                coef[e, ((s - 1) * 2 + d) * PAD : ((s - 1) * 2 + d) * PAD + rows] = w

    gates, ups, downs = wg, wu, wd

    def up(e, rows_of, count):
        gate = up_ = None
        for p in range(PIECES):
            r = rows_of(p)
            ks = slice(p * part, (p + 1) * part)
            g, u = mm(r, gates[e, ks, :]), mm(r, ups[e, ks, :])
            gate, up_ = (g, u) if gate is None else (gate + g, up_ + u)
        hidden[0:count] = (silu(gate) * up_).astype(BF16)

    def shared_up():
        for load in loads[0:2]:
            load.wait()
        up(0, lambda p: slots[half - 1, 1, p], PAD)

    def shared_down():
        loads[2].wait()
        out = mm(hidden[0:PAD], downs[0])[0:rows]
        base[...] = mid_ref[...] + out.astype(BF16).astype(F32)

    def expert_up(e, b):
        up(e + 1, lambda p: slots[pl.ds(2 * b, 2), :, p].reshape(4 * PAD, part), 4 * PAD)

    def expert_down(e, b):
        cf = coef[e, pl.ds(pl.multiple_of(b * (4 * PAD), 4 * PAD), 4 * PAD), :]
        for p in range(PIECES):
            for c in range(0, part, 512):
                o = mm(hidden[...], downs[e + 1, :, p * part + c : p * part + c + 512])
                o = o.astype(BF16).astype(F32) * cf
                if e == 0:
                    first[:, p * part + c : p * part + c + 512] = o
                else:
                    o = o + first[:, p * part + c : p * part + c + 512]
                    contrib[pl.ds(2 * b, 2), :, p, :, c : c + 512] = o.astype(BF16).reshape(2, 2, PAD, 512)

    def forward(s, p):
        gather.wait(s, p)
        if not (isinstance(s, int) and s == half):
            gather.start(s + 1, p)

    def turn(s, work):
        for i in range(2):
            for p in range(i * PIECES // 2, (i + 1) * PIECES // 2):
                forward(s, p)
            work[i]()

    turn(1, (shared_up, shared_down))
    for p in range(PIECES):
        forward(2, p)
    for load in loads[3:]:
        load.wait()

    def pair(b, carry):
        for e in range(2):
            turn(2 * b + 3 + e, (functools.partial(expert_up, e, b), functools.partial(expert_down, e, b)))
        return carry

    lax.fori_loop(0, half // 2 - 2, pair, 0)
    b = half // 2 - 2
    for e in range(2):
        turn(2 * b + 3 + e, (functools.partial(expert_up, e, b), functools.partial(expert_down, e, b)))
    b = half // 2 - 1
    for e in range(2):
        expert_up(e, b)
        expert_down(e, b)

    def passed(t, d, p, source):
        return rcopy(
            contrib.at[source - 1, 0 if isinstance(source, int) and source == half else d, p, pl.ds(0, rows)],
            arrive.at[t, d, p, pl.ds(0, rows)],
            r_send.at[t, d, p],
            r_recv.at[t, d, p],
            at(-1 if d == 0 else 1),
        )

    def begins(d, p):
        return (p < PIECES // 2) == (d == 0)

    for p in range(PIECES):
        for d in range(2):
            if begins(d, p):
                passed(0, d, p, half).start()
            else:
                passed(1, d, p, half - 1).start()

    def relay(t, d, p):
        passed(t - 1, d, p, half - t).wait_recv()
        mine = contrib[half - t - 1, d, p, 0:rows].astype(F32)
        contrib[half - t - 1, d, p, 0:rows] = (mine + arrive[t - 1, d, p, 0:rows].astype(F32)).astype(BF16)
        passed(t, d, p, half - t).start()

    for p in range(PIECES):
        for d in range(2):
            if begins(d, p):
                relay(1, d, p)

    def hop(t, carry):
        for p in range(PIECES):
            for d in range(2):
                relay(t, d, p)
        return carry

    lax.fori_loop(2, half, hop, 0)
    for p in range(PIECES):
        for d in range(2):
            passed(half - 1, d, p, 1).wait_recv()
        got = arrive[half - 1, 0, p, 0:rows].astype(F32) + arrive[half - 1, 1, p, 0:rows].astype(F32)
        total = base[:, p * part : (p + 1) * part] + contrib[half - 1, 1, p, 0:rows].astype(F32) + got
        out_ref[:, p * part : (p + 1) * part] = total.astype(BF16)
    gather.drain()
    for p in range(PIECES):
        for d in range(2):
            for t in range(half):
                if t > 0 or begins(d, p):
                    passed(t, d, p, half - t).wait_send()


VM = pl.BlockSpec(memory_space=pltpu.VMEM)
HBM = pl.BlockSpec(memory_space=pltpu.HBM)
DMA = pltpu.SemaphoreType.DMA


def far(array):
    return pltpu.with_memory_space_constraint(array, pltpu.HBM)


def cost(us):
    return pl.CostEstimate(flops=int(us * 2e8), bytes_accessed=int(us * 3e6), transcendentals=0)


def per_device(
    residual_input,
    attention_norm_gain,
    receptance_weight,
    key_weight,
    value_weight,
    decay_weight,
    correction_rate_weight,
    output_gate_weight,
    decay_offset,
    correction_rate_offset,
    self_term_weight,
    head_read_gain,
    previous_state,
    attention_output_weight,
    feedforward_norm_gain,
    routes,
    routing_weight,
    routed_gate_weight,
    routed_up_weight,
    routed_down_weight,
    common_gate_weight,
    common_up_weight,
    common_down_weight,
):
    size = lax.axis_size("ep")
    half = size // 4
    rows, width = residual_input.shape
    part = width // PIECES
    cols = receptance_weight.shape[1]
    lanes = ROLES * cols
    big = pltpu.CompilerParams
    two = 2 * HEAD_SIZE
    square = HEAD_SIZE * HEAD_SIZE
    landed, blk, exp_m, red_m, sib_gate, sib_up, sib_down = pl.pallas_call(
        functools.partial(project_kernel, size),
        out_shape=(
            jax.ShapeDtypeStruct((size // 2, rows, 2 * lanes), BF16),
            jax.ShapeDtypeStruct((256, 256), BF16),
            jax.ShapeDtypeStruct((two, square), BF16),
            jax.ShapeDtypeStruct((square, two), BF16),
            pltpu.HBM(routed_gate_weight.shape, BF16),
            pltpu.HBM(routed_up_weight.shape, BF16),
            pltpu.HBM(routed_down_weight.shape, BF16),
        ),
        in_specs=[VM, VM] + [HBM] * 9,
        out_specs=(VM,) * 4 + (HBM,) * 3,
        scratch_shapes=[
            pltpu.VMEM((2 * lanes, width), BF16),
            pltpu.VMEM((width, 2 * lanes), BF16),
            pltpu.VMEM((half, 2, PIECES, PAD, part), BF16),
            pltpu.VMEM((half, 2, PAD, 2 * lanes), BF16),
            pltpu.VMEM((size // 2, rows, 2 * lanes), BF16),
            DMA((ROLES,)),
            DMA((ROLES + 3,)),
            DMA((ROLES + 3,)),
            DMA((half, 2, PIECES)),
            DMA((half, 2, PIECES)),
            DMA((half, 2)),
            DMA((half, 2)),
        ],
        compiler_params=big(collective_id=0, has_side_effects=True, vmem_limit_bytes=16 << 20),
        cost_estimate=cost(40),
        name="project",
    )(
        residual_input,
        attention_norm_gain.reshape(1, width),
        far(receptance_weight.T),
        far(key_weight.T),
        far(value_weight.T),
        far(decay_weight.T),
        far(correction_rate_weight.T),
        far(output_gate_weight.T),
        far(routed_gate_weight),
        far(routed_up_weight),
        far(routed_down_weight),
    )
    prm = jnp.stack((decay_offset, correction_rate_offset, self_term_weight, head_read_gain)).reshape(
        4, HEAD_COUNT, HEAD_SIZE
    )
    total = rows * HEAD_COUNT
    blocks = (rows // TOKEN_BLOCK, TOKEN_BLOCK, HEAD_COUNT, square)
    next_state, middle = pl.pallas_call(
        state_kernel,
        out_shape=(
            jax.ShapeDtypeStruct(previous_state.shape, F32),
            jax.ShapeDtypeStruct((rows, width), F32),
        ),
        in_specs=[VM] * 6 + [HBM] * 2,
        out_specs=(HBM, VM),
        scratch_shapes=[
            pltpu.VMEM(blocks, F32),
            pltpu.VMEM(blocks, F32),
            pltpu.VMEM(attention_output_weight.shape, BF16),
            pltpu.VMEM((3, total, two), F32),
            pltpu.VMEM((3, total, two), F32),
            pltpu.VMEM((4, total, two), F32),
            pltpu.VMEM((total, two), BF16),
            pltpu.VMEM((total, two), F32),
            pltpu.VMEM((total, two), F32),
            pltpu.VMEM((total, two), F32),
            pltpu.VMEM((rows, HEAD_COUNT * HEAD_SIZE), F32),
            DMA(blocks[:1]),
            DMA(blocks[:1]),
            DMA,
        ],
        compiler_params=big(vmem_limit_bytes=40 << 20),
        cost_estimate=cost(8),
        name="state",
    )(landed, blk, exp_m, red_m, prm, residual_input, far(attention_output_weight), far(previous_state))
    inner = routed_gate_weight.shape[2]
    hidden_out = pl.pallas_call(
        functools.partial(expert_kernel, size),
        out_shape=jax.ShapeDtypeStruct((rows, width), BF16),
        in_specs=[VM] * 4 + [HBM] * 9,
        out_specs=VM,
        scratch_shapes=[
            pltpu.VMEM((3, width, inner), BF16),
            pltpu.VMEM((3, width, inner), BF16),
            pltpu.VMEM((3, inner, width), BF16),
            pltpu.VMEM((half, 2, PIECES, PAD, part), BF16),
            pltpu.VMEM((half, 2, PIECES, PAD, part), BF16),
            pltpu.VMEM((half, 2, PIECES, PAD, part), BF16),
            pltpu.VMEM((4 * PAD, inner), BF16),
            pltpu.VMEM((4 * PAD, width), F32),
            pltpu.VMEM((2, 2 * half * PAD, 1), F32),
            pltpu.VMEM((rows, width), F32),
            DMA((3, 3)),
            DMA((half, 2, PIECES)),
            DMA((half, 2, PIECES)),
            DMA((half, 2, PIECES)),
            DMA((half, 2, PIECES)),
        ],
        compiler_params=big(collective_id=1, has_side_effects=True, vmem_limit_bytes=38 << 20),
        cost_estimate=cost(50),
        name="experts",
    )(
        middle,
        feedforward_norm_gain.reshape(1, width),
        routes,
        routing_weight,
        far(routed_gate_weight),
        far(routed_up_weight),
        far(routed_down_weight),
        far(sib_gate),
        far(sib_up),
        far(sib_down),
        far(common_gate_weight),
        far(common_up_weight),
        far(common_down_weight),
    )
    return (hidden_out, next_state)


def solution(mesh):
    return jax.shard_map(
        per_device,
        mesh=mesh,
        in_specs=(
            P(("grp", "ep"), None),
            P(),
            P(None, "ep"),
            P(None, "ep"),
            P(None, "ep"),
            P(None, "ep"),
            P(None, "ep"),
            P(None, "ep"),
            P(),
            P(),
            P(),
            P(),
            P(("grp", "ep"), None, None),
            P(),
            P(),
            P("grp", None),
            P("grp", None),
            P("ep", None, None),
            P("ep", None, None),
            P("ep", None, None),
            P(),
            P(),
            P(),
        ),
        out_specs=(P(("grp", "ep"), None), P(("grp", "ep"), None, None)),
        check_vma=False,
    )
```
